512 devices in a mesh: ep: 32 (over z, core), tp: 16 (over y, x).
Axes of the slice: x: 4, y: 4, z: 16, core: 2. Of those that a mesh axis runs over, the one named last changes fastest.
Arguments:
- tokens: bfloat16 [1024, 2048], P('ep'), may hold values from -6 to 6
- recurrent_head_state: float32 [1024, 16, 4096], P('ep', 'tp'), may hold values from -4 to 4
- first_norm_gain: float32 [2048], replicated, may hold values from 0.1 to 1.9
- receptance_matrix: bfloat16 [2048, 1024], P(None, 'tp'), may hold values from -0.125 to 0.125
- key_matrix: bfloat16 [2048, 1024], P(None, 'tp'), may hold values from -0.125 to 0.125
- value_matrix: bfloat16 [2048, 1024], P(None, 'tp'), may hold values from -0.125 to 0.125
- decay_matrix: bfloat16 [2048, 1024], P(None, 'tp'), may hold values from -0.125 to 0.125
- decay_offset: float32 [1024], P('tp'), may hold values from -3 to 0.5
- correction_offset: float32 [1024], P('tp'), may hold values from -2 to 2
- correction_key_factor: float32 [1024], P('tp'), may hold values from -1 to 1
- own_term_weight: float32 [1024], P('tp'), may hold values from -0.9 to 0.9
- head_norm_gain: float32 [1024], P('tp'), may hold values from 0.1 to 1.9
- output_matrix: bfloat16 [1024, 2048], P('tp'), may hold values from -0.1875 to 0.1875
- second_norm_gain: float32 [2048], replicated, may hold values from 0.1 to 1.9
- routing: int32 [1024, 2], replicated, may hold values from 0 to 31, all different within a row; in each aligned block of 32 rows (0 to 31, 32 to 63, ...) at most 4 rows name the same one
- routing_weight: float32 [1024, 2], P('ep'), may hold values from 0.1 to 1
- expert_gate_weight: bfloat16 [32, 2048, 4096], P('ep', None, 'tp'), may hold values from -0.125 to 0.125
- expert_up_weight: bfloat16 [32, 2048, 4096], P('ep', None, 'tp'), may hold values from -0.125 to 0.125
- expert_down_weight: bfloat16 [32, 4096, 2048], P('ep', 'tp'), may hold values from -0.125 to 0.125
- dense_gate_weight: bfloat16 [2048, 2816], P(None, 'ep'), may hold values from -0.125 to 0.125
- dense_up_weight: bfloat16 [2048, 2816], P(None, 'ep'), may hold values from -0.125 to 0.125
- dense_down_weight: bfloat16 [2816, 2048], P('ep'), may hold values from -0.109375 to 0.109375
- dense_gate_offset: float32 [2048], replicated, may hold values from -3 to 3
Outputs:
- layer_out: bfloat16 [1024, 2048], P(('ep', 'tp'))
- next_state: float32 [1024, 16, 4096], P('ep', 'tp')
The draws below stay inside these ranges and needn't reach their ends.
Inputs may be any that keep to these rules, and one draw needn't show every extreme that they name: `routing`: each row names 2 different experts. In each aligned block of 32 rows no expert is named more than 4 times, a bound that some block reaches.
All inputs are finite; a program needn't handle non-finite values.
Results may differ from the reference program's by a relative error of at most 0.017.
Values may be sent and summed in bfloat16 or wider, within the bound.
A program may use at most 64 MiB of HBM per device.

```python
import math
from functools import partial
import jax
import jax.numpy as jnp
import numpy as np
from jax import lax

D = 2048
HEAD_COUNT = 16
HEAD_WIDTH = 64
FF_E = 4096
FF_D = 2816
TOP_K = 2
B_DEV = 32
B_TOT = 1024
EXPERTS = 32
CAP = 4
N_EP = 32


def strengthened(entries, rng, source, target, parts, factor):
    def block_of(axis_at):
        return (jnp.arange(entries.shape[axis_at]) // (entries.shape[axis_at] // parts)).reshape((-1,) + (1,) * (entries.ndim - 1 - axis_at))

    first = jax.random.permutation(rng, parts)[block_of(target)]
    second = (block_of(target) + parts // 2) % parts
    return jnp.where((block_of(source) == first) | (block_of(source) == second), factor * entries, entries)


def levels(rng, extent, pieces, smallest, high):
    level, own = 1.0, jax.random.fold_in(rng, 6)
    for position, blocks in pieces:
        draws = jnp.exp(jax.random.uniform(jax.random.fold_in(own, position), (blocks,), jnp.float32, smallest / len(pieces), high / len(pieces)))
        level = level * jnp.repeat(draws, extent[position] // blocks).reshape([-1 if axis == position else 1 for axis in range(len(extent))])
    return level


def shared_out(stream_key, own, number, rows, amount, top, most, lean):
    sequence = jax.random.permutation(stream_key, amount)
    crowded, common = shares(amount, rows * top, most, lean, True), shares(amount, rows * top, most, lean, False)
    places = jnp.arange(amount)

    def named(tallies, turn):
        used = int((tallies > 0).sum())
        fixed = max(1, used // 4)
        moved = fixed + (places - fixed + turn * (used - fixed)) % max(1, amount - fixed)
        return jnp.zeros((amount,), jnp.int32).at[sequence[jnp.where(places < fixed, places, moved)]].set(jnp.asarray(tallies, jnp.int32))

    tallies = jnp.where(number % 4 == 0, named(crowded, number // 4), named(common, number - number // 4 - 1))
    mixed = jax.random.permutation(jax.random.fold_in(own, 3), amount)
    giver, receiver = mixed[0:amount // 2 * 2:2], mixed[1:amount // 2 * 2:2]
    room = jnp.minimum(tallies[giver] - 1, most - tallies[receiver]) // 2
    room = jnp.where((giver == sequence[0]) | (receiver == sequence[0]) | (tallies[receiver] == 0), 0, jnp.maximum(room, 0))
    moved = jax.random.randint(jax.random.fold_in(own, 4), (amount // 2,), 0, 1 << 20) % (room + 1)
    tallies = tallies.at[giver].add(-moved).at[receiver].add(moved)
    labels = jnp.searchsorted(jnp.cumsum(tallies), jnp.arange(rows * top), side="right").astype(jnp.int32)
    listing = labels.reshape(top, rows).T
    listing = listing[jax.random.permutation(jax.random.fold_in(own, 1), rows)]
    turn = jax.random.randint(jax.random.fold_in(own, 2), (rows, 1), 0, top)
    return jnp.take_along_axis(listing, (jnp.arange(top)[None, :] + turn) % top, axis=1)


def shares(amount, total, reach, slope, full):
    weights = [(1 << 20) // math.isqrt(grade ** slope) + 1 for grade in range(1, amount + 1)]
    largest = reach if full else min(reach, max(-(-total // amount), total * weights[0] // sum(weights)))
    least = 1 if total - largest >= amount - 1 else 0
    counts, spare = [largest] + [least] * (amount - 1), total - largest - least * (amount - 1)
    while spare > 0:
        movable = [i for i in range(1, amount) if counts[i] < largest] or [i for i in range(1, amount) if counts[i] < reach]
        pool, left = sum([weights[i] for i in movable]), spare
        for i in movable:
            extra = min(reach - counts[i], max(1, left * weights[i] // pool), spare)
            counts[i] = counts[i] + extra
            spare = spare - extra
    return np.array(counts)


def bell_draw(stream_key, dims, width, limit, split=(), kind=jnp.bfloat16):
    entries = jax.random.normal(stream_key, dims, jnp.float32) * width
    if len(split) > 0:
        entries = levels(stream_key, dims, split, -0.22, 0.18) * entries
    return jnp.clip(entries, min=-limit, max=limit).astype(kind)


def gaussian_with(rng, dims, scale, limit, pieces, heavy, kind=jnp.bfloat16):
    drawn = scale * jax.random.normal(rng, dims, jnp.float32)
    if pieces:
        drawn = drawn * levels(rng, dims, pieces, -0.22, 0.18)
    return jnp.clip(strengthened(drawn, jax.random.fold_in(rng, 3), *heavy), -limit, limit).astype(kind)


def setup_inputs(seed: int = 0) -> dict:
    streams_of = jax.random.split(jax.random.key(seed), 24)
    tokens = bell_draw(streams_of[0], (B_TOT, D), 1.0, 6.0, ((0, 32),))
    recurrent_head_state = bell_draw(streams_of[1], (B_TOT, HEAD_COUNT, HEAD_WIDTH * HEAD_WIDTH), 0.5, 4.0, ((0, 32), (1, 16)), jnp.float32)
    first_norm_gain = jnp.clip(1.0 + 0.18 * jax.random.normal(streams_of[2], (D,), jnp.float32), 0.1, 1.9)
    receptance_matrix = bell_draw(streams_of[3], (D, HEAD_COUNT * HEAD_WIDTH), D ** -0.5, 0.125, ((1, 16),))
    key_matrix = bell_draw(streams_of[4], (D, HEAD_COUNT * HEAD_WIDTH), D ** -0.5, 0.125, ((1, 16),))
    value_matrix = bell_draw(streams_of[5], (D, HEAD_COUNT * HEAD_WIDTH), D ** -0.5, 0.125, ((1, 16),))
    decay_matrix = bell_draw(streams_of[6], (D, HEAD_COUNT * HEAD_WIDTH), D ** -0.5, 0.125, ((1, 16),))
    decay_offset = jnp.clip(-3.0 + 3.5 * jax.random.uniform(streams_of[7], (HEAD_COUNT * HEAD_WIDTH,), jnp.float32) ** levels(streams_of[7], (HEAD_COUNT * HEAD_WIDTH,), ((0, 16),), -0.2, 0.2), -3.0, 0.5)
    correction_offset = jnp.clip(jax.random.uniform(streams_of[8], (HEAD_COUNT * HEAD_WIDTH,), jnp.float32, -2.0, 2.0) * levels(streams_of[8], (HEAD_COUNT * HEAD_WIDTH,), ((0, 16),), -0.4, 0.0), -2.0, 2.0)
    correction_key_factor = jnp.clip(jax.random.uniform(streams_of[9], (HEAD_COUNT * HEAD_WIDTH,), jnp.float32, -1.0, 1.0) * levels(streams_of[9], (HEAD_COUNT * HEAD_WIDTH,), ((0, 16),), -0.4, 0.0), -1.0, 1.0)
    own_term_weight = bell_draw(streams_of[10], (HEAD_COUNT * HEAD_WIDTH,), 0.15, 0.9, ((0, 16),), jnp.float32)
    head_norm_gain = jnp.clip(1.0 + 0.18 * jax.random.normal(streams_of[11], (HEAD_COUNT * HEAD_WIDTH,), jnp.float32), 0.1, 1.9)
    output_matrix = bell_draw(streams_of[12], (HEAD_COUNT * HEAD_WIDTH, D), (HEAD_COUNT * HEAD_WIDTH) ** -0.5, 0.1875, ((0, 16),))
    second_norm_gain = jnp.clip(1.0 + 0.18 * jax.random.normal(streams_of[13], (D,), jnp.float32), 0.1, 1.9)
    routing_keys = jax.random.split(jax.random.fold_in(streams_of[14], 1), B_TOT // B_DEV)
    routing_turns = jax.random.permutation(jax.random.fold_in(streams_of[14], 3), B_TOT // B_DEV)
    routing = jax.vmap(lambda own, number: shared_out(jax.random.fold_in(streams_of[14], 2), own, number, B_DEV, EXPERTS, TOP_K, CAP, 2))(routing_keys, routing_turns).reshape((B_TOT, TOP_K))
    routing_weight = jnp.clip(0.1 + 0.9 * jax.random.uniform(streams_of[15], (B_TOT, TOP_K), jnp.float32) ** levels(streams_of[15], (B_TOT, TOP_K), ((0, 32),), -0.2, 0.2), 0.1, 1.0)
    expert_gate_weight = bell_draw(streams_of[16], (EXPERTS, D, FF_E), D ** -0.5, 0.125, ((0, 32), (2, 16)))
    expert_up_weight = bell_draw(streams_of[17], (EXPERTS, D, FF_E), D ** -0.5, 0.125, ((0, 32), (2, 16)))
    expert_down_weight = gaussian_with(streams_of[18], (EXPERTS, FF_E, D), FF_E ** -0.5, 0.125, ((0, 32), (1, 16)), (1, 2, 16, 2.0))
    dense_gate_weight = bell_draw(streams_of[19], (D, FF_D), D ** -0.5, 0.125, ((1, 32),))
    dense_up_weight = bell_draw(streams_of[20], (D, FF_D), D ** -0.5, 0.125, ((1, 32),))
    dense_down_weight = bell_draw(streams_of[21], (FF_D, D), FF_D ** -0.5, 0.109375, ((0, 32),))
    dense_gate_offset = jnp.clip(jax.random.uniform(streams_of[22], (D,), jnp.float32, -3.0, 3.0), -3.0, 3.0)
    return {"tokens": tokens, "recurrent_head_state": recurrent_head_state, "first_norm_gain": first_norm_gain, "receptance_matrix": receptance_matrix, "key_matrix": key_matrix, "value_matrix": value_matrix, "decay_matrix": decay_matrix, "decay_offset": decay_offset, "correction_offset": correction_offset, "correction_key_factor": correction_key_factor, "own_term_weight": own_term_weight, "head_norm_gain": head_norm_gain, "output_matrix": output_matrix, "second_norm_gain": second_norm_gain, "routing": routing, "routing_weight": routing_weight, "expert_gate_weight": expert_gate_weight, "expert_up_weight": expert_up_weight, "expert_down_weight": expert_down_weight, "dense_gate_weight": dense_gate_weight, "dense_up_weight": dense_up_weight, "dense_down_weight": dense_down_weight, "dense_gate_offset": dense_gate_offset}


PRECISE = lax.Precision.HIGHEST

def rms_scale(rows, gain):
    floats = rows.astype(jnp.float32)
    return floats * lax.rsqrt(lax.optimization_barrier(jnp.mean(floats * floats, axis=-1, keepdims=True)) + 1e-06) * gain

def route_table(block_routes, experts, capacity):
    flat_routes = block_routes.reshape(-1)
    chosen = (flat_routes[:, None] == jnp.arange(experts, dtype=jnp.int32)[None, :]).astype(jnp.int32)
    before = jnp.cumsum(chosen, axis=0, dtype=jnp.int32) - chosen
    slot_index = lax.optimization_barrier(jnp.sum(before * chosen, axis=1))
    slot_match = (slot_index[:, None] == jnp.arange(capacity, dtype=jnp.int32)[None, :]).astype(jnp.float32)
    dispatch_table = chosen.astype(jnp.float32)[:, :, None] * slot_match[:, None, :]
    return dispatch_table.reshape(block_routes.shape[0], block_routes.shape[1], experts, capacity)

def state_update(receptance_rows, key_matrix_rows, value_matrix_rows, decay_logits, recurrent_head_state, decay_offset, correction_offset, correction_key_factor, own_term_weight, head_norm_gain, head_width):
    seq_count = key_matrix_rows.shape[0]
    decay_factor = jnp.exp(-jnp.exp(decay_offset + decay_logits))
    in_rate = jax.nn.sigmoid(correction_offset + correction_key_factor * key_matrix_rows)
    key_in = key_matrix_rows * in_rate

    def split_heads(block):
        return block.reshape(seq_count, -1, head_width)
    keys_head = split_heads(key_matrix_rows)
    unit_keys = keys_head * lax.rsqrt(lax.optimization_barrier(jnp.mean(keys_head * keys_head, axis=-1, keepdims=True)) + 1e-06) * head_width ** (-0.5)
    rate_head = split_heads(in_rate)
    head_keys = split_heads(key_in)
    decay_head = split_heads(decay_factor)
    head_values = split_heads(value_matrix_rows)
    head_receptance = split_heads(receptance_rows)
    matrix = recurrent_head_state.reshape(seq_count, -1, head_width, head_width)
    removed = jnp.einsum('bhvk,bhk->bhv', matrix, unit_keys, precision=PRECISE)
    updated = matrix * decay_head[:, :, None, :] - removed[..., None] * (unit_keys * rate_head)[:, :, None, :] + head_values[..., None] * head_keys[:, :, None, :]
    readout = jnp.einsum('bhvk,bhk->bhv', updated, head_receptance, precision=PRECISE)
    center = lax.optimization_barrier(jnp.mean(readout, axis=-1, keepdims=True))
    spread = lax.optimization_barrier(jnp.mean(jnp.square(readout - center), axis=-1, keepdims=True))
    normalized_rows = (readout - center) * lax.rsqrt(spread + 0.00064) * head_norm_gain.reshape(-1, head_width)
    own_term_total = lax.optimization_barrier(jnp.sum(head_receptance * head_keys * own_term_weight.reshape(-1, head_width), axis=-1, keepdims=True))
    normalized_rows = normalized_rows + own_term_total * head_values
    return (normalized_rows.reshape(seq_count, -1).astype(jnp.bfloat16), updated.reshape(seq_count, -1, head_width * head_width))

def reference(tokens, recurrent_head_state, first_norm_gain, receptance_matrix, key_matrix, value_matrix, decay_matrix, decay_offset, correction_offset, correction_key_factor, own_term_weight, head_norm_gain, output_matrix, second_norm_gain, routing, routing_weight, expert_gate_weight, expert_up_weight, expert_down_weight, dense_gate_weight, dense_up_weight, dense_down_weight, dense_gate_offset):
    normalized_rows = rms_scale(tokens, first_norm_gain).astype(jnp.bfloat16)
    receptance_rows = jnp.dot(normalized_rows, receptance_matrix, preferred_element_type=jnp.float32)
    key_matrix_rows = jnp.dot(normalized_rows, key_matrix, preferred_element_type=jnp.float32)
    value_matrix_rows = jnp.dot(normalized_rows, value_matrix, preferred_element_type=jnp.float32)
    decay_logits = jnp.dot(normalized_rows, decay_matrix, preferred_element_type=jnp.float32)
    head_outputs, next_state = state_update(receptance_rows, key_matrix_rows, value_matrix_rows, decay_logits, recurrent_head_state, decay_offset, correction_offset, correction_key_factor, own_term_weight, head_norm_gain, HEAD_WIDTH)
    hidden_sum = tokens.astype(jnp.float32) + jnp.dot(head_outputs, output_matrix, preferred_element_type=jnp.float32)
    ffn_in = rms_scale(hidden_sum, second_norm_gain).astype(jnp.bfloat16)
    tables = jax.vmap(partial(route_table, experts=EXPERTS, capacity=CAP))(routing.reshape(N_EP, B_DEV, TOP_K))
    grouped = ffn_in.reshape(N_EP, B_DEV, D).astype(jnp.float32)
    buffers = jnp.einsum('sbkec,sbd->escd', tables, grouped, precision=PRECISE).astype(jnp.bfloat16)

    def one_expert(packed):
        rows, gate_part, up_part, down_part = packed
        flat_rows = rows.reshape(-1, D)
        gate_pre = jnp.dot(flat_rows, gate_part, preferred_element_type=jnp.float32)
        up_pre = jnp.dot(flat_rows, up_part, preferred_element_type=jnp.float32)
        hidden = (jax.nn.silu(gate_pre) * up_pre).astype(jnp.bfloat16)
        result = jnp.dot(hidden, down_part, preferred_element_type=jnp.float32).astype(jnp.bfloat16)
        return result.reshape(rows.shape)
    expert_outs = lax.map(one_expert, (buffers, expert_gate_weight, expert_up_weight, expert_down_weight))
    weighted = jnp.einsum('sbkec,sbk->secb', tables, routing_weight.reshape(N_EP, B_DEV, TOP_K), precision=PRECISE)
    moe = jnp.einsum('secb,escd->sbd', weighted, expert_outs.astype(jnp.float32), precision=PRECISE).reshape(B_TOT, D)
    dense_hidden = (jax.nn.silu(jnp.dot(ffn_in, dense_gate_weight, preferred_element_type=jnp.float32)) * jnp.dot(ffn_in, dense_up_weight, preferred_element_type=jnp.float32)).astype(jnp.bfloat16)
    block_units = FF_D // N_EP

    def add_block(total, index):
        start = index * block_units
        piece = lax.dynamic_slice_in_dim(dense_hidden, start, block_units, 1)
        rows = lax.dynamic_slice_in_dim(dense_down_weight, start, block_units, 0)
        part = jnp.dot(piece, rows, preferred_element_type=jnp.float32).astype(jnp.bfloat16)
        part = lax.optimization_barrier(part)
        return (total + part.astype(jnp.float32), None)
    dense_sum, _ = lax.scan(add_block, jnp.zeros((B_TOT, D), jnp.float32), jnp.arange(N_EP, dtype=jnp.int32))
    layer_out = (hidden_sum + moe + jax.nn.sigmoid(dense_gate_offset) * dense_sum).astype(jnp.bfloat16)
    return (layer_out, next_state)
```

```python
import functools

import jax
import jax.numpy as jnp
from jax import lax
from jax.experimental import pallas as pl
from jax.experimental.pallas import tpu as pltpu
from jax.sharding import PartitionSpec as P

HEAD_WIDTH = 64
MESH = pl.DeviceIdType.MESH
F32 = jnp.float32
BF16 = jnp.bfloat16


def sigmoid(x):
    return 1.0 / (1.0 + jnp.exp(-x))


def layer_kernel(sizes, *refs):
    groups, lanes, seqs, width, experts, cap = sizes
    per_lane = seqs // lanes
    part = width // lanes
    pair = 2 * HEAD_WIDTH
    tiles = HEAD_WIDTH // 2
    (
        tokens_hbm, state_hbm, gain1_hbm, wr_hbm, wk_hbm, wv_hbm, wd_hbm,
        doff_hbm, coff_hbm, ckey_hbm, own_hbm, hgain_hbm, wout_hbm, gain2_hbm,
        routes_hbm, rweight_hbm, eg_hbm, eu_hbm, ed_hbm, dg_hbm, du_hbm, dd_hbm, goff_hbm,
        out_ref, next_hbm,
        tok, state, gain1, joined, doff, coff, ckey, own, hgain, wout, gain2,
        routes, rweight, eg, eu, ed, dense_up, dd, goff,
        next_state, tokf, wide, slots,
        col_send, row_send, col_in, row_in, hidden,
        disp_send, disp_in, rows_all, dense_send, dense_in, dense_rows, dback_send, dback_in,
        eo_send, eo_in, back_send, back_in, moe_send, moe_in, moe_wide,
        load_sem, store_sem, send_sem, recv_sem,
    ) = refs
    g = lax.axis_index("ep")
    t = lax.axis_index("tp")
    my_part = pl.ds(pl.multiple_of(t * part, part), part)

    wr, wk, wv, wd = (joined.at[pl.ds(i * HEAD_WIDTH, HEAD_WIDTH)] for i in range(4))
    units = dg_hbm.shape[0]
    dg, du = (dense_up.at[pl.ds(i * 128, units)] for i in range(2))
    sources = (
        tokens_hbm, gain1_hbm, wr_hbm, wk_hbm, wv_hbm, wd_hbm, doff_hbm, coff_hbm, ckey_hbm, own_hbm, hgain_hbm,
        state_hbm, wout_hbm, routes_hbm, rweight_hbm, gain2_hbm, eg_hbm, eu_hbm, dg_hbm, du_hbm, ed_hbm, dd_hbm, goff_hbm,
    )
    targets = (
        tok, gain1, wr, wk, wv, wd, doff, coff, ckey, own, hgain,
        state, wout, routes, rweight, gain2, eg, eu, dg, du, ed, dd, goff,
    )
    loads = {
        id(to): pltpu.make_async_copy(frm, to, load_sem.at[i])
        for i, (frm, to) in enumerate(zip(sources, targets))
    }
    for to in targets:
        loads[id(to)].start()

    def arrived(*buffers):
        for to in buffers:
            loads[id(to)].wait()

    barrier = pltpu.get_barrier_semaphore()

    @pl.loop(1, lanes)
    def _(p):
        pl.semaphore_signal(barrier, inc=1, device_id=(g, lax.rem(t + p, lanes)), device_id_type=MESH)

    @pl.loop(1, groups)
    def _(p):
        pl.semaphore_signal(barrier, inc=1, device_id=(lax.rem(g + p, groups), t), device_id_type=MESH)

    def over_lanes(stage, source, target):
        @pl.loop(1, lanes)
        def _(p):
            peer = lax.rem(t + p, lanes)
            pltpu.make_async_remote_copy(
                src_ref=source(peer), dst_ref=target, send_sem=send_sem.at[stage],
                recv_sem=recv_sem.at[stage], device_id=(g, peer), device_id_type=MESH,
            ).start()

    def over_groups(stage, source, target):
        @pl.loop(1, groups)
        def _(p):
            peer = lax.rem(g + p, groups)
            pltpu.make_async_remote_copy(
                src_ref=source(peer), dst_ref=target, send_sem=send_sem.at[stage],
                recv_sem=recv_sem.at[stage], device_id=(peer, t), device_id_type=MESH,
            ).start()

    def descriptor(stage, ref):
        return pltpu.make_async_remote_copy(
            src_ref=ref, dst_ref=ref, send_sem=send_sem.at[stage], recv_sem=recv_sem.at[stage],
            device_id=(g, lax.rem(t + 1, lanes)), device_id_type=MESH,
        )

    arrived(tok, gain1)
    floats = tok[...].astype(F32)
    tokf[...] = floats
    normed = (
        floats * lax.rsqrt(jnp.mean(floats * floats, axis=-1, keepdims=True) + 1e-06) * gain1[...]
    ).astype(BF16)
    arrived(wr, wk, wv, wd)
    projected = lax.dot_general(normed, joined[...], (((1,), (1,)), ((), ())), preferred_element_type=F32)
    recept = projected[:, 0:HEAD_WIDTH]
    keys = projected[:, HEAD_WIDTH : 2 * HEAD_WIDTH]
    values = projected[:, 2 * HEAD_WIDTH : 3 * HEAD_WIDTH]
    decay_pre = projected[:, 3 * HEAD_WIDTH : 4 * HEAD_WIDTH]

    arrived(doff, coff, ckey, own, hgain)
    decay = jnp.exp(-jnp.exp(doff[...] + decay_pre))
    rate = sigmoid(coff[...] + ckey[...] * keys)
    key_in = keys * rate
    unit = keys * lax.rsqrt(jnp.mean(keys * keys, axis=-1, keepdims=True) + 1e-06) * HEAD_WIDTH**-0.5

    def twice(x):
        return jnp.concatenate([x, x], axis=1)

    decay2, unit2, rate2, key2, recept2, values2 = map(
        twice, (decay, unit, unit * rate, key_in, recept, values)
    )
    lane_of = lax.broadcasted_iota(jnp.int32, (seqs, pair), 1)
    low = lane_of < HEAD_WIDTH

    def halves(x):
        first = jnp.sum(jnp.where(low, x, 0.0), axis=-1, keepdims=True)
        second = jnp.sum(jnp.where(low, 0.0, x), axis=-1, keepdims=True)
        return first, second

    def picked(x, lane):
        return jnp.sum(jnp.where(lane_of == lane, x, 0.0), axis=-1, keepdims=True)

    arrived(state)
    at_once = 4

    def some_tiles(step, readout):
        for inner in range(at_once):
            c = step * at_once + inner
            rows = pl.ds(c, seqs, stride=tiles)
            block = state[rows, :]
            removed = jnp.where(low, *halves(block * unit2))
            added = jnp.where(low, picked(values2, 2 * c), picked(values2, 2 * c + 1))
            block = block * decay2 - removed * rate2 + added * key2
            next_state[rows, :] = block
            first, second = halves(block * recept2)
            readout = jnp.where(lane_of == 2 * c, first, readout)
            readout = jnp.where(lane_of == 2 * c + 1, second, readout)
        return readout

    readout = lax.fori_loop(0, tiles // at_once, some_tiles, jnp.zeros((seqs, pair), F32))
    store = pltpu.make_async_copy(next_state, next_hbm, store_sem)
    store.start()
    readout = readout[:, 0:HEAD_WIDTH]
    center = jnp.mean(readout, axis=-1, keepdims=True)
    spread = jnp.mean(jnp.square(readout - center), axis=-1, keepdims=True)
    heads = (readout - center) * lax.rsqrt(spread + 0.00064) * hgain[...]
    heads = heads + jnp.sum(recept * key_in * own[...], axis=-1, keepdims=True) * values
    heads = heads.astype(BF16)

    arrived(wout)
    share = jnp.dot(heads, wout[...], preferred_element_type=F32)
    wide[0:seqs, :] = share
    col_send[...] = share.astype(BF16)
    col_in[pl.ds(t, 1)] = col_send[:, my_part][None]
    pl.semaphore_wait(barrier, lanes + groups - 2)
    over_lanes(
        0, lambda peer: col_send.at[:, pl.ds(pl.multiple_of(peer * part, part), part)], col_in.at[t]
    )
    for p in range(lanes):
        row_send[p] = wide[p * per_lane : (p + 1) * per_lane, :].astype(BF16)
    row_in[pl.ds(t, 1)] = row_send[pl.ds(t, 1)]
    over_lanes(1, lambda peer: row_send.at[peer], row_in.at[t])

    arrived(routes, rweight)
    chunk = pl.ds(pl.multiple_of(g // (128 // seqs) * 128, 128), 128)
    offset = lax.rem(g, 128 // seqs) * seqs
    pick = (
        lax.broadcasted_iota(jnp.int32, (128, seqs), 0)
        == lax.broadcasted_iota(jnp.int32, (128, seqs), 1) + offset
    ).astype(BF16)
    own_routes = jnp.dot(
        routes[:, chunk].astype(F32).astype(BF16), pick, preferred_element_type=F32
    ).astype(jnp.int32)
    slot = lax.broadcasted_iota(jnp.int32, (experts * cap, seqs), 0)
    expert_of, place_of = slot // cap, lax.rem(slot, cap)
    first, second = own_routes[0:1] == expert_of, own_routes[1:2] == expert_of
    either = jnp.where(first | second, 1.0, 0.0).astype(BF16)
    earlier = (
        lax.broadcasted_iota(jnp.int32, (seqs, seqs), 0)
        < lax.broadcasted_iota(jnp.int32, (seqs, seqs), 1)
    ).astype(BF16)
    here = jnp.dot(either, earlier, preferred_element_type=F32).astype(jnp.int32) == place_of
    table = jnp.where((first | second) & here, 1.0, 0.0).astype(BF16)
    weighted = jnp.where(first & here, rweight[0:1], 0.0) + jnp.where(second & here, rweight[1:2], 0.0)

    mine = (
        lax.broadcasted_iota(jnp.int32, (per_lane, seqs), 1)
        == lax.broadcasted_iota(jnp.int32, (per_lane, seqs), 0) + t * per_lane
    ).astype(BF16)
    hidden[...] = jnp.dot(mine, tok[...], preferred_element_type=F32)

    arrived(gain2)
    descriptor(0, col_in.at[pl.ds(0, lanes - 1)]).wait_recv()
    total = tokf[:, my_part]
    for p in range(lanes):
        total = total + col_in[p].astype(F32)
    gained = (total * gain2[:, my_part]).astype(BF16)
    slots[...] = jnp.dot(table, gained, preferred_element_type=F32)
    for e in range(experts):
        disp_send[e] = slots[e * cap : (e + 1) * cap, :].astype(BF16)
    disp_in[pl.ds(g, 1)] = disp_send[pl.ds(g, 1)]
    over_groups(2, lambda peer: disp_send.at[peer], disp_in.at[g])

    descriptor(1, row_in.at[pl.ds(0, lanes - 1)]).wait_recv()
    total = hidden[...]
    for p in range(lanes):
        total = total + row_in[p].astype(F32)
    hidden[...] = total
    dense_send[...] = (
        total * lax.rsqrt(jnp.mean(total * total, axis=-1, keepdims=True) + 1e-06) * gain2[...]
    ).astype(BF16)
    dense_in[pl.ds(g, 1)] = dense_send[...][None]
    over_groups(3, lambda peer: dense_send, dense_in.at[g])

    descriptor(2, disp_in.at[pl.ds(0, groups - 1)]).wait_recv()
    for e in range(groups):
        slots[e * cap : (e + 1) * cap, :] = disp_in[e].astype(F32)
    rows_all[:, my_part] = slots[...].astype(BF16)
    over_lanes(4, lambda peer: rows_all.at[:, my_part], rows_all.at[:, my_part])

    inverse = 1.0 / (gain2[...] * gain2[...])
    arrived(eg, eu, ed)
    descriptor(4, rows_all.at[:, pl.ds(0, width - part)]).wait_recv()
    squares = jnp.zeros((groups * cap, part), F32)
    for p in range(lanes):
        piece = rows_all[:, p * part : (p + 1) * part].astype(F32)
        squares = squares + piece * piece * inverse[:, p * part : (p + 1) * part]
    scale = lax.rsqrt(jnp.sum(squares, axis=-1, keepdims=True) / width + 1e-06)
    gate = jnp.dot(rows_all[...], eg[0], preferred_element_type=F32) * scale
    up = jnp.dot(rows_all[...], eu[0], preferred_element_type=F32) * scale
    inner = (gate * sigmoid(gate) * up).astype(BF16)
    block = 2 * part
    for p in range(width // block):
        eo_send[:, p * block : (p + 1) * block] = jnp.dot(
            inner, ed[0, :, p * block : (p + 1) * block], preferred_element_type=F32
        ).astype(BF16)
    eo_in[pl.ds(t, 1)] = eo_send[:, my_part][None]
    over_lanes(
        5, lambda peer: eo_send.at[:, pl.ds(pl.multiple_of(peer * part, part), part)], eo_in.at[t]
    )

    arrived(dg, du, dd, goff)
    descriptor(3, dense_in.at[pl.ds(0, groups - 1)]).wait_recv()
    for e in range(groups):
        wide[e * per_lane : (e + 1) * per_lane, :] = dense_in[e].astype(F32)
    dense_rows[...] = wide[...].astype(BF16)
    both = lax.dot_general(
        dense_rows[...], dense_up[...], (((1,), (1,)), ((), ())), preferred_element_type=F32
    )
    gate, up = both[:, 0:units], both[:, 128 : 128 + units]
    inner = (gate * sigmoid(gate) * up).astype(BF16)
    wide[...] = jnp.dot(inner, dd[...], preferred_element_type=F32)
    for e in range(groups):
        dback_send[e] = wide[e * per_lane : (e + 1) * per_lane, :].astype(BF16)
    dback_in[pl.ds(g, 1)] = dback_send[pl.ds(g, 1)]

    descriptor(5, eo_in.at[pl.ds(0, lanes - 1)]).wait_recv()
    total = jnp.zeros((groups * cap, part), F32)
    for p in range(lanes):
        total = total + eo_in[p].astype(F32)
    slots[...] = total
    for e in range(groups):
        back_send[e] = slots[e * cap : (e + 1) * cap, :].astype(BF16)
    back_in[pl.ds(g, 1)] = back_send[pl.ds(g, 1)]
    over_groups(6, lambda peer: back_send.at[peer], back_in.at[g])
    over_groups(7, lambda peer: dback_send.at[peer], dback_in.at[g])

    upper = weighted.astype(BF16)
    lower = (weighted - upper.astype(F32)).astype(BF16)
    descriptor(6, back_in.at[pl.ds(0, groups - 1)]).wait_recv()
    for e in range(experts):
        slots[e * cap : (e + 1) * cap, :] = back_in[e].astype(F32)
    back = slots[...].astype(BF16)
    across = (((0,), (0,)), ((), ()))
    moe = lax.dot_general(upper, back, across, preferred_element_type=F32)
    moe = moe + lax.dot_general(lower, back, across, preferred_element_type=F32)
    slots[0:seqs, :] = moe
    for p in range(lanes):
        moe_send[p] = slots[p * per_lane : (p + 1) * per_lane, :]
    moe_in[pl.ds(t, 1)] = moe_send[pl.ds(t, 1)]
    over_lanes(8, lambda peer: moe_send.at[peer], moe_in.at[t])

    descriptor(7, dback_in.at[pl.ds(0, groups - 1)]).wait_recv()
    total = jnp.zeros((per_lane, width), F32)
    for e in range(groups):
        total = total + dback_in[e].astype(F32)
    base = hidden[...] + sigmoid(goff[...]) * total
    descriptor(8, moe_in.at[pl.ds(0, lanes - 1)]).wait_recv()
    for p in range(lanes):
        moe_wide[:, p * part : (p + 1) * part] = moe_in[p]
    out_ref[...] = (base + moe_wide[...]).astype(BF16)

    store.wait()
    descriptor(0, col_in.at[pl.ds(0, lanes - 1)]).wait_send()
    descriptor(1, row_in.at[pl.ds(0, lanes - 1)]).wait_send()
    descriptor(2, disp_in.at[pl.ds(0, groups - 1)]).wait_send()
    descriptor(3, dense_in.at[pl.ds(0, groups - 1)]).wait_send()
    descriptor(4, rows_all.at[:, pl.ds(0, width - part)]).wait_send()
    descriptor(5, eo_in.at[pl.ds(0, lanes - 1)]).wait_send()
    descriptor(6, back_in.at[pl.ds(0, groups - 1)]).wait_send()
    descriptor(7, dback_in.at[pl.ds(0, groups - 1)]).wait_send()
    descriptor(8, moe_in.at[pl.ds(0, lanes - 1)]).wait_send()


def local(*args):
    (
        tokens, state, gain1, wr, wk, wv, wd, doff, coff, ckey, own, hgain, wout, gain2,
        routing, rweight, eg, eu, ed, dg, du, dd, goff,
    ) = args
    groups, lanes = lax.axis_size("ep"), lax.axis_size("tp")
    seqs, width = tokens.shape
    top = routing.shape[1]
    experts = groups
    cap = 2 * seqs * top // experts
    per_lane, part = seqs // lanes, width // lanes
    rows = seqs * HEAD_WIDTH * HEAD_WIDTH // 128
    row = lambda v: v.reshape(1, -1)
    operands = (
        tokens, state.reshape(rows, 128), row(gain1), wr.T, wk.T, wv.T, wd.T, row(doff), row(coff), row(ckey), row(own),
        row(hgain), wout, row(gain2), routing.T, rweight.T, eg, eu, ed, dg.T, du.T, dd, row(goff),
    )
    vmem = pltpu.VMEM
    joined, dense_up = vmem((4 * HEAD_WIDTH, width), BF16), vmem((256, width), BF16)
    held = [vmem(a.shape, a.dtype) for a in operands]
    held = [*held[:3], joined, *held[7:19], dense_up, *held[21:]]
    sizes = (groups, lanes, seqs, width, experts, cap)
    scratch = held + [
        vmem((rows, 128), F32),
        vmem((seqs, width), F32),
        vmem((max(seqs, groups * per_lane), width), F32),
        vmem((groups * cap, part), F32),
        vmem((seqs, width), BF16),
        vmem((lanes, per_lane, width), BF16),
        vmem((lanes, seqs, part), BF16),
        vmem((lanes, per_lane, width), BF16),
        vmem((per_lane, width), F32),
        vmem((experts, cap, part), BF16),
        vmem((groups, cap, part), BF16),
        vmem((groups * cap, width), BF16),
        vmem((per_lane, width), BF16),
        vmem((groups, per_lane, width), BF16),
        vmem((groups * per_lane, width), BF16),
        vmem((groups, per_lane, width), BF16),
        vmem((groups, per_lane, width), BF16),
        vmem((groups * cap, width), BF16),
        vmem((lanes, groups * cap, part), BF16),
        vmem((groups, cap, part), BF16),
        vmem((experts, cap, part), BF16),
        vmem((lanes, per_lane, part), F32),
        vmem((lanes, per_lane, part), F32),
        vmem((per_lane, width), F32),
        pltpu.SemaphoreType.DMA((len(operands),)),
        pltpu.SemaphoreType.DMA,
        pltpu.SemaphoreType.DMA((9,)),
        pltpu.SemaphoreType.DMA((9,)),
    ]
    layer_out, next_state = pl.pallas_call(
        functools.partial(layer_kernel, sizes),
        out_shape=(
            jax.ShapeDtypeStruct((per_lane, width), BF16),
            jax.ShapeDtypeStruct((rows, 128), F32),
        ),
        in_specs=[pl.BlockSpec(memory_space=pl.ANY)] * len(operands),
        out_specs=(pl.BlockSpec(memory_space=pltpu.VMEM), pl.BlockSpec(memory_space=pl.ANY)),
        scratch_shapes=scratch,
        compiler_params=pltpu.CompilerParams(
            collective_id=0, has_side_effects=True, vmem_limit_bytes=60_000_000
        ),
        name="layer",
    )(*operands)
    return layer_out, next_state.reshape(state.shape)


def solution(mesh):
    return jax.shard_map(
        local,
        mesh=mesh,
        in_specs=(
            P("ep", None),
            P("ep", "tp", None),
            P(),
            P(None, "tp"),
            P(None, "tp"),
            P(None, "tp"),
            P(None, "tp"),
            P("tp"),
            P("tp"),
            P("tp"),
            P("tp"),
            P("tp"),
            P("tp", None),
            P(),
            P(),
            P("ep", None),
            P("ep", None, "tp"),
            P("ep", None, "tp"),
            P("ep", "tp", None),
            P(None, "ep"),
            P(None, "ep"),
            P("ep", None),
            P(),
        ),
        out_specs=(P(("ep", "tp"), None), P("ep", "tp", None)),
        check_vma=False,
    )
```

```python
import functools

import jax
import jax.numpy as jnp
from jax import lax
from jax.experimental import pallas as pl
from jax.experimental.pallas import tpu as pltpu
from jax.sharding import PartitionSpec as P

HEAD_WIDTH = 64
MESH = pl.DeviceIdType.MESH
F32 = jnp.float32
BF16 = jnp.bfloat16


def sigmoid(x):
    return 1.0 / (1.0 + jnp.exp(-x))


def layer_kernel(sizes, *refs):
    groups, lanes, seqs, width, experts, cap = sizes
    per_lane = seqs // lanes
    part = width // lanes
    pair = 2 * HEAD_WIDTH
    tiles = HEAD_WIDTH // 2
    (
        tokens_hbm, state_hbm, gain1_hbm, wr_hbm, wk_hbm, wv_hbm, wd_hbm,
        doff_hbm, coff_hbm, ckey_hbm, own_hbm, hgain_hbm, wout_hbm, gain2_hbm,
        routes_hbm, rweight_hbm, eg_hbm, eu_hbm, ed_hbm, dg_hbm, du_hbm, dd_hbm, goff_hbm,
        out_ref, next_state,
        tok, state, gain1, joined, doff, coff, ckey, own, hgain, wout, gain2,
        routes, rweight, eg, eu, ed, dense_up, dd, goff,
        wide, slots,
        col_send, row_send, col_in, row_in, hidden,
        disp_send, disp_in, rows_all, dense_send, dense_in, dense_rows, dback_send, dback_in, pair_in, chip_sum,
        eo_send, eo_in, back_send, back_in, moe_send, moe_in, moe_wide,
        load_sem, send_sem, recv_sem,
    ) = refs
    g = lax.axis_index("ep")
    t = lax.axis_index("tp")
    chips, chip, core = groups // 2, g // 2, lax.rem(g, 2)
    partner = g + 1 - 2 * core
    quarter, half = chips // 4, groups * cap // 2
    my_part = pl.ds(pl.multiple_of(t * part, part), part)

    barrier = pltpu.get_barrier_semaphore()

    @pl.loop(1, lanes)
    def _(p):
        pl.semaphore_signal(barrier, inc=1, device_id=(g, lax.rem(t + p, lanes)), device_id_type=MESH)

    @pl.loop(1, groups)
    def _(p):
        pl.semaphore_signal(barrier, inc=1, device_id=(lax.rem(g + p, groups), t), device_id_type=MESH)

    wr, wk, wv, wd = (joined.at[pl.ds(i * HEAD_WIDTH, HEAD_WIDTH)] for i in range(4))
    units = dg_hbm.shape[0]
    dg, du = (dense_up.at[pl.ds(i * 128, units)] for i in range(2))
    sources = (
        tokens_hbm, gain1_hbm, wr_hbm, wk_hbm, wv_hbm, wd_hbm, doff_hbm, coff_hbm, ckey_hbm, own_hbm, hgain_hbm,
        state_hbm, wout_hbm, routes_hbm, rweight_hbm, gain2_hbm, eg_hbm, eu_hbm, dg_hbm, du_hbm, ed_hbm, dd_hbm, goff_hbm,
    )
    targets = (
        tok, gain1, wr, wk, wv, wd, doff, coff, ckey, own, hgain,
        state, wout, routes, rweight, gain2, eg, eu, dg, du, ed, dd, goff,
    )
    loads = {
        id(to): pltpu.make_async_copy(frm, to, load_sem.at[i])
        for i, (frm, to) in enumerate(zip(sources, targets))
    }
    for to in targets:
        loads[id(to)].start()

    def arrived(*buffers):
        for to in buffers:
            loads[id(to)].wait()

    def over_lanes(stage, source, target):
        @pl.loop(1, lanes)
        def _(p):
            peer = lax.rem(t + p, lanes)
            pltpu.make_async_remote_copy(
                src_ref=source(peer), dst_ref=target, send_sem=send_sem.at[stage],
                recv_sem=recv_sem.at[stage], device_id=(g, peer), device_id_type=MESH,
            ).start()

    def to_device(stage, source, target, peer):
        pltpu.make_async_remote_copy(
            src_ref=source, dst_ref=target, send_sem=send_sem.at[stage],
            recv_sem=recv_sem.at[stage], device_id=(peer, t), device_id_type=MESH,
        ).start()

    def to_experts():
        @pl.loop(chips // 2, chips)
        def _(j):
            for c in range(2):
                peer = lax.rem(chip + quarter - j + chips, chips) * 2 + c
                to_device(3, disp_send.at[peer], disp_in.at[2 * j + core], peer)

        @pl.loop(1, chips // 2)
        def _(k):
            j = lax.rem(quarter + k, chips // 2)
            for c in range(2):
                peer = lax.rem(chip + quarter - j + chips, chips) * 2 + c
                to_device(2, disp_send.at[peer], disp_in.at[2 * j + core], peer)

        to_device(2, disp_send.at[partner], disp_in.at[2 * quarter + core], partner)

    def to_groups_near():
        @pl.loop(1, chips // 2)
        def _(k):
            j = lax.rem(quarter + k, chips // 2)
            for c in range(2):
                peer = lax.rem(chip + j - quarter + chips, chips) * 2 + c
                to_device(8, back_send.at[2 * j + c], back_in.at[g], peer)

        to_device(8, back_send.at[2 * quarter + 1 - core], back_in.at[g], partner)

    def to_groups_far():
        @pl.loop(chips // 2, chips)
        def _(j):
            for c in range(2):
                peer = lax.rem(chip + j - quarter + chips, chips) * 2 + c
                to_device(8, back_send.at[2 * j + c], back_in.at[g], peer)

    def over_chips(stage, source, target):
        def send(distance):
            peer = lax.rem(chip + distance, chips)
            to_device(stage, source(peer), target, 2 * peer + core)

        send(chips // 2)

        @pl.loop(1, chips // 2)
        def _(k):
            send(chips // 2 - k)
            send(chips // 2 + k)

    def descriptor(stage, ref):
        return pltpu.make_async_remote_copy(
            src_ref=ref, dst_ref=ref, send_sem=send_sem.at[stage], recv_sem=recv_sem.at[stage],
            device_id=(g, lax.rem(t + 1, lanes)), device_id_type=MESH,
        )

    arrived(tok, gain1)
    floats = tok[...].astype(F32)
    normed = (
        floats * lax.rsqrt(jnp.mean(floats * floats, axis=-1, keepdims=True) + 1e-06) * gain1[...]
    ).astype(BF16)
    arrived(wr, wk, wv, wd)
    projected = lax.dot_general(normed, joined[...], (((1,), (1,)), ((), ())), preferred_element_type=F32)
    recept = projected[:, 0:HEAD_WIDTH]
    keys = projected[:, HEAD_WIDTH : 2 * HEAD_WIDTH]
    values = projected[:, 2 * HEAD_WIDTH : 3 * HEAD_WIDTH]
    decay_pre = projected[:, 3 * HEAD_WIDTH : 4 * HEAD_WIDTH]

    arrived(doff, coff, ckey, own, hgain)
    decay = jnp.exp(-jnp.exp(doff[...] + decay_pre))
    rate = sigmoid(coff[...] + ckey[...] * keys)
    key_in = keys * rate
    unit = keys * lax.rsqrt(jnp.mean(keys * keys, axis=-1, keepdims=True) + 1e-06) * HEAD_WIDTH**-0.5

    def twice(x):
        return jnp.concatenate([x, x], axis=1)

    decay2, unit2, rate2, key2, recept2, values2 = map(
        twice, (decay, unit, unit * rate, key_in, recept, values)
    )
    lane_of = lax.broadcasted_iota(jnp.int32, (seqs, pair), 1)
    low = lane_of < HEAD_WIDTH

    def halves(x):
        first = jnp.sum(jnp.where(low, x, 0.0), axis=-1, keepdims=True)
        second = jnp.sum(jnp.where(low, 0.0, x), axis=-1, keepdims=True)
        return first, second

    def picked(x, lane):
        return jnp.sum(jnp.where(lane_of == lane, x, 0.0), axis=-1, keepdims=True)

    arrived(state)
    at_once = 4

    def some_tiles(step, readout):
        for inner in range(at_once):
            c = step * at_once + inner
            rows = pl.ds(c, seqs, stride=tiles)
            block = state[rows, :]
            removed = jnp.where(low, *halves(block * unit2))
            added = jnp.where(low, picked(values2, 2 * c), picked(values2, 2 * c + 1))
            block = block * decay2 - removed * rate2 + added * key2
            next_state[rows, :] = block
            first, second = halves(block * recept2)
            readout = jnp.where(lane_of == 2 * c, first, readout)
            readout = jnp.where(lane_of == 2 * c + 1, second, readout)
        return readout

    readout = lax.fori_loop(0, tiles // at_once, some_tiles, jnp.zeros((seqs, pair), F32))
    readout = readout[:, 0:HEAD_WIDTH]
    center = jnp.mean(readout, axis=-1, keepdims=True)
    spread = jnp.mean(jnp.square(readout - center), axis=-1, keepdims=True)
    heads = (readout - center) * lax.rsqrt(spread + 0.00064) * hgain[...]
    heads = heads + jnp.sum(recept * key_in * own[...], axis=-1, keepdims=True) * values
    heads = heads.astype(BF16)

    arrived(wout)
    col_send[...] = jnp.dot(heads, wout[...], preferred_element_type=F32).astype(BF16)
    col_in[pl.ds(t, 1)] = col_send[:, my_part][None]
    pl.semaphore_wait(barrier, lanes + groups - 2)
    over_lanes(
        0, lambda peer: col_send.at[:, pl.ds(pl.multiple_of(peer * part, part), part)], col_in.at[t]
    )

    arrived(routes, rweight)
    chunk = pl.ds(pl.multiple_of(g // (128 // seqs) * 128, 128), 128)
    offset = lax.rem(g, 128 // seqs) * seqs
    pick = (
        lax.broadcasted_iota(jnp.int32, (128, seqs), 0)
        == lax.broadcasted_iota(jnp.int32, (128, seqs), 1) + offset
    ).astype(BF16)
    own_routes = jnp.dot(
        routes[:, chunk].astype(F32).astype(BF16), pick, preferred_element_type=F32
    ).astype(jnp.int32)
    slot = lax.broadcasted_iota(jnp.int32, (experts * cap, seqs), 0)
    expert_of, place_of = slot // cap, lax.rem(slot, cap)
    first, second = own_routes[0:1] == expert_of, own_routes[1:2] == expert_of
    either = jnp.where(first | second, 1.0, 0.0).astype(BF16)
    earlier = (
        lax.broadcasted_iota(jnp.int32, (seqs, seqs), 0)
        < lax.broadcasted_iota(jnp.int32, (seqs, seqs), 1)
    ).astype(BF16)
    here = jnp.dot(either, earlier, preferred_element_type=F32).astype(jnp.int32) == place_of
    table = jnp.where((first | second) & here, 1.0, 0.0).astype(BF16)
    weighted = jnp.where(first & here, rweight[0:1], 0.0) + jnp.where(second & here, rweight[1:2], 0.0)

    arrived(gain2)
    descriptor(0, col_in.at[pl.ds(0, lanes - 1)]).wait_recv()
    total = tok[:, my_part].astype(F32)
    for p in range(lanes):
        total = total + col_in[p].astype(F32)
    gained = (total * gain2[:, my_part]).astype(BF16)
    slots[...] = jnp.dot(table, gained, preferred_element_type=F32)
    for e in range(experts):
        disp_send[e] = slots[e * cap : (e + 1) * cap, :].astype(BF16)
    disp_in[pl.ds(2 * quarter + core, 1)] = disp_send[pl.ds(g, 1)]
    to_experts()
    slots[0:seqs, :] = total
    for p in range(lanes):
        row_send[p] = slots[p * per_lane : (p + 1) * per_lane, :]
    row_in[pl.ds(t, 1)] = row_send[pl.ds(t, 1)]
    over_lanes(1, lambda peer: row_send.at[peer], row_in.at[t])

    def whole_rows(stage, side):
        for e in range(chips * side, chips * (side + 1)):
            slots[e * cap : (e + 1) * cap, :] = disp_in[e].astype(F32)
        rows = slice(side * half, (side + 1) * half)
        rows_all[rows, my_part] = slots[rows, :].astype(BF16)
        mine = rows_all.at[pl.ds(side * half, half), my_part]
        over_lanes(stage, lambda peer: mine, mine)

    descriptor(2, disp_in.at[pl.ds(0, chips - 1)]).wait_recv()
    whole_rows(4, 0)

    descriptor(1, row_in.at[pl.ds(0, lanes - 1)]).wait_recv()
    for p in range(lanes):
        hidden[:, p * part : (p + 1) * part] = row_in[p]
    total = hidden[...]
    dense_send[...] = (
        total * lax.rsqrt(jnp.mean(total * total, axis=-1, keepdims=True) + 1e-06) * gain2[...]
    ).astype(BF16)
    dense_in[pl.ds(core * chips + chip, 1)] = dense_send[...][None]
    over_chips(9, lambda peer: dense_send, dense_in.at[core * chips + chip])

    descriptor(3, disp_in.at[pl.ds(chips, chips)]).wait_recv()
    whole_rows(5, 1)

    inverse = 1.0 / (gain2[...] * gain2[...])

    def expert(stage, side):
        rows = slice(side * half, (side + 1) * half)
        squares = jnp.zeros((half, part), F32)
        for p in range(lanes):
            piece = rows_all[rows, p * part : (p + 1) * part].astype(F32)
            squares = squares + piece * piece * inverse[:, p * part : (p + 1) * part]
        scale = lax.rsqrt(jnp.sum(squares, axis=-1, keepdims=True) / width + 1e-06)
        gate = jnp.dot(rows_all[rows, :], eg[0], preferred_element_type=F32) * scale
        up = jnp.dot(rows_all[rows, :], eu[0], preferred_element_type=F32) * scale
        inner = (gate * sigmoid(gate) * up).astype(BF16)
        block = 2 * part
        for p in range(width // block):
            eo_send[rows, p * block : (p + 1) * block] = jnp.dot(
                inner, ed[0, :, p * block : (p + 1) * block], preferred_element_type=F32
            ).astype(BF16)
        eo_in[pl.ds(t, 1), rows] = eo_send[rows, my_part][None]
        over = pl.ds(side * half, half)
        over_lanes(
            stage,
            lambda peer: eo_send.at[over, pl.ds(pl.multiple_of(peer * part, part), part)],
            eo_in.at[t, over],
        )

    arrived(eg, eu, ed)
    descriptor(4, rows_all.at[pl.ds(0, half), pl.ds(0, width - part)]).wait_recv()
    expert(6, 0)
    descriptor(5, rows_all.at[pl.ds(0, half), pl.ds(0, width - part)]).wait_recv()
    expert(7, 1)

    my_half, other_half = pl.ds(core * chips, chips), pl.ds((1 - core) * chips, chips)
    descriptor(9, dense_in.at[pl.ds(0, chips - 1)]).wait_recv()
    to_device(10, dense_in.at[my_half], dense_in.at[my_half], partner)
    arrived(dg, du, dd, goff)
    descriptor(10, dense_in.at[pl.ds(0, chips)]).wait_recv()
    for e in range(groups):
        wide[e * per_lane : (e + 1) * per_lane, :] = dense_in[e].astype(F32)
    dense_rows[...] = wide[...].astype(BF16)
    both = lax.dot_general(
        dense_rows[...], dense_up[...], (((1,), (1,)), ((), ())), preferred_element_type=F32
    )
    gate, up = both[:, 0:units], both[:, 128 : 128 + units]
    inner = (gate * sigmoid(gate) * up).astype(BF16)
    wide[...] = jnp.dot(inner, dd[...], preferred_element_type=F32)
    for e in range(groups):
        dback_send[e] = wide[e * per_lane : (e + 1) * per_lane, :].astype(BF16)
    to_device(11, dback_send.at[other_half], pair_in, partner)

    def expert_sums(side):
        rows = slice(side * half, (side + 1) * half)
        total = jnp.zeros((half, part), F32)
        for p in range(lanes):
            total = total + eo_in[p, rows].astype(F32)
        slots[rows, :] = total
        for e in range(chips * side, chips * (side + 1)):
            back_send[e] = slots[e * cap : (e + 1) * cap, :].astype(BF16)

    descriptor(6, eo_in.at[pl.ds(0, lanes - 1), pl.ds(0, half)]).wait_recv()
    expert_sums(0)
    back_in[pl.ds(g, 1)] = back_send[pl.ds(2 * quarter + core, 1)]
    to_groups_near()
    descriptor(11, pair_in).wait_recv()
    chip_sum[...] = (dback_send[my_half].astype(F32) + pair_in[...].astype(F32)).astype(BF16)
    dback_in[pl.ds(chip, 1)] = chip_sum[pl.ds(chip, 1)]
    descriptor(7, eo_in.at[pl.ds(0, lanes - 1), pl.ds(0, half)]).wait_recv()
    expert_sums(1)
    to_groups_far()

    over_chips(12, lambda peer: chip_sum.at[peer], dback_in.at[chip])

    upper = weighted.astype(BF16)
    lower = (weighted - upper.astype(F32)).astype(BF16)
    descriptor(8, back_in.at[pl.ds(0, groups - 1)]).wait_recv()
    for e in range(experts):
        slots[e * cap : (e + 1) * cap, :] = back_in[e].astype(F32)
    back = slots[...].astype(BF16)
    across = (((0,), (0,)), ((), ()))
    moe = lax.dot_general(upper, back, across, preferred_element_type=F32)
    moe = moe + lax.dot_general(lower, back, across, preferred_element_type=F32)
    slots[0:seqs, :] = moe
    for p in range(lanes):
        moe_send[p] = slots[p * per_lane : (p + 1) * per_lane, :]
    moe_in[pl.ds(t, 1)] = moe_send[pl.ds(t, 1)]
    over_lanes(13, lambda peer: moe_send.at[peer], moe_in.at[t])

    descriptor(12, dback_in.at[pl.ds(0, chips - 1)]).wait_recv()
    total = jnp.zeros((per_lane, width), F32)
    for e in range(chips):
        total = total + dback_in[e].astype(F32)
    total = hidden[...] + sigmoid(goff[...]) * total
    descriptor(13, moe_in.at[pl.ds(0, lanes - 1)]).wait_recv()
    for p in range(lanes):
        moe_wide[:, p * part : (p + 1) * part] = moe_in[p]
    out_ref[...] = (total + moe_wide[...]).astype(BF16)

    over_half = rows_all.at[pl.ds(0, half), pl.ds(0, width - part)]
    sums_half = eo_in.at[pl.ds(0, lanes - 1), pl.ds(0, half)]
    sent = (
        col_in.at[pl.ds(0, lanes - 1)], row_in.at[pl.ds(0, lanes - 1)],
        disp_in.at[pl.ds(0, chips - 1)], disp_in.at[pl.ds(0, chips)], over_half, over_half, sums_half, sums_half,
        back_in.at[pl.ds(0, groups - 1)], dense_in.at[pl.ds(0, chips - 1)], dense_in.at[pl.ds(0, chips)], pair_in,
        dback_in.at[pl.ds(0, chips - 1)], moe_in.at[pl.ds(0, lanes - 1)],
    )
    for stage, ref in enumerate(sent):
        descriptor(stage, ref).wait_send()


def finish_kernel(out_vmem, next_vmem, out_hbm, next_hbm, sems):
    copies = (
        pltpu.make_async_copy(next_vmem, next_hbm, sems.at[0]),
        pltpu.make_async_copy(out_vmem, out_hbm, sems.at[1]),
    )
    for copy in copies:
        copy.start()
    for copy in copies:
        copy.wait()


def local(*args):
    (
        tokens, state, gain1, wr, wk, wv, wd, doff, coff, ckey, own, hgain, wout, gain2,
        routing, rweight, eg, eu, ed, dg, du, dd, goff,
    ) = args
    groups, lanes = lax.axis_size("ep"), lax.axis_size("tp")
    seqs, width = tokens.shape
    top = routing.shape[1]
    experts = groups
    cap = 2 * seqs * top // experts
    per_lane, part = seqs // lanes, width // lanes
    rows = seqs * HEAD_WIDTH * HEAD_WIDTH // 128
    row = lambda v: v.reshape(1, -1)
    operands = (
        tokens, state.reshape(rows, 128), row(gain1), wr.T, wk.T, wv.T, wd.T, row(doff), row(coff), row(ckey), row(own),
        row(hgain), wout, row(gain2), routing.T, rweight.T, eg, eu, ed, dg.T, du.T, dd, row(goff),
    )
    vmem = pltpu.VMEM
    joined, dense_up = vmem((4 * HEAD_WIDTH, width), BF16), vmem((256, width), BF16)
    held = [vmem(a.shape, a.dtype) for a in operands]
    held = [*held[:3], joined, *held[7:19], dense_up, *held[21:]]
    sizes = (groups, lanes, seqs, width, experts, cap)
    scratch = held + [
        vmem((groups * per_lane, width), F32),
        vmem((groups * cap, part), F32),
        vmem((seqs, width), BF16),
        vmem((lanes, per_lane, part), F32),
        vmem((lanes, seqs, part), BF16),
        vmem((lanes, per_lane, part), F32),
        vmem((per_lane, width), F32),
        vmem((experts, cap, part), BF16),
        vmem((groups, cap, part), BF16),
        vmem((groups * cap, width), BF16),
        vmem((per_lane, width), BF16),
        vmem((groups, per_lane, width), BF16),
        vmem((groups * per_lane, width), BF16),
        vmem((groups, per_lane, width), BF16),
        vmem((groups // 2, per_lane, width), BF16),
        vmem((groups // 2, per_lane, width), BF16),
        vmem((groups // 2, per_lane, width), BF16),
        vmem((groups * cap, width), BF16),
        vmem((lanes, groups * cap, part), BF16),
        vmem((groups, cap, part), BF16),
        vmem((experts, cap, part), BF16),
        vmem((lanes, per_lane, part), F32),
        vmem((lanes, per_lane, part), F32),
        vmem((per_lane, width), F32),
        pltpu.SemaphoreType.DMA((len(operands),)),
        pltpu.SemaphoreType.DMA((14,)),
        pltpu.SemaphoreType.DMA((14,)),
    ]
    layer_out, next_state = pl.pallas_call(
        functools.partial(layer_kernel, sizes),
        out_shape=(vmem((per_lane, width), BF16), vmem((rows, 128), F32)),
        in_specs=[pl.BlockSpec(memory_space=pltpu.HBM)] * len(operands),
        out_specs=[pl.BlockSpec(memory_space=pltpu.VMEM)] * 2,
        scratch_shapes=scratch,
        compiler_params=pltpu.CompilerParams(
            collective_id=0, has_side_effects=True, vmem_limit_bytes=60_000_000
        ),
        name="layer",
    )(*operands)
    layer_out, next_state = pl.pallas_call(
        finish_kernel,
        out_shape=(
            jax.ShapeDtypeStruct((per_lane, width), BF16),
            jax.ShapeDtypeStruct((rows, 128), F32),
        ),
        in_specs=[pl.BlockSpec(memory_space=pltpu.VMEM)] * 2,
        out_specs=[pl.BlockSpec(memory_space=pltpu.HBM)] * 2,
        scratch_shapes=[pltpu.SemaphoreType.DMA((2,))],
        compiler_params=pltpu.CompilerParams(vmem_limit_bytes=2_000_000),
        name="finish",
    )(layer_out, next_state)
    return layer_out, next_state.reshape(state.shape)


def solution(mesh):
    return jax.shard_map(
        local,
        mesh=mesh,
        in_specs=(
            P("ep", None),
            P("ep", "tp", None),
            P(),
            P(None, "tp"),
            P(None, "tp"),
            P(None, "tp"),
            P(None, "tp"),
            P("tp"),
            P("tp"),
            P("tp"),
            P("tp"),
            P("tp"),
            P("tp", None),
            P(),
            P(),
            P("ep", None),
            P("ep", None, "tp"),
            P("ep", None, "tp"),
            P("ep", "tp", None),
            P(None, "ep"),
            P(None, "ep"),
            P("ep", None),
            P(),
        ),
        out_specs=(P(("ep", "tp"), None), P("ep", "tp", None)),
        check_vma=False,
    )
```

```python
import functools

import jax
import jax.numpy as jnp
from jax import lax
from jax.experimental import pallas as pl
from jax.experimental.pallas import tpu as pltpu
from jax.sharding import PartitionSpec as P

HEAD_WIDTH = 64
MESH = pl.DeviceIdType.MESH
F32 = jnp.float32
BF16 = jnp.bfloat16
ENDS = (6, 12, 16)
PARTS = len(ENDS)
COLUMNS, ROWS, DENSE, PASS_ON, PAIR, BLOCKS, RETURN, FINAL, DISPATCH = range(9)
GATHER = DISPATCH + PARTS
SUMS = GATHER + PARTS
STAGES = SUMS + PARTS


def sigmoid(x):
    return 1.0 / (1.0 + jnp.exp(-x))


def layer_kernel(sizes, *refs):
    groups, lanes, seqs, width, experts, cap = sizes
    per_lane = seqs // lanes
    part = width // lanes
    pair = 2 * HEAD_WIDTH
    tiles = HEAD_WIDTH // 2
    (
        tokens_hbm, state_hbm, gain1_hbm, wr_hbm, wk_hbm, wv_hbm, wd_hbm,
        doff_hbm, coff_hbm, ckey_hbm, own_hbm, hgain_hbm, wout_hbm, gain2_hbm,
        routes_hbm, rweight_hbm, eg_hbm, eu_hbm, ed_hbm, dg_hbm, du_hbm, dd_hbm, goff_hbm,
        out_ref, next_state,
        tok, state, gain1, joined, doff, coff, ckey, own, hgain, wout, gain2,
        routes, rweight, eg, eu, ed, dense_up, dd, goff,
        wide, slots,
        col_send, row_send, col_in, row_in, hidden,
        disp_send, disp_in, rows_all, dense_send, dense_in, dense_rows, dback_send, dback_in, pair_in, chip_sum,
        eo_send, eo_in, back_send, back_in, moe_send, moe_in, moe_wide,
        load_sem, send_sem, recv_sem, go,
    ) = refs
    g = lax.axis_index("ep")
    t = lax.axis_index("tp")
    chips, chip, core = groups // 2, g // 2, lax.rem(g, 2)
    partner = g + 1 - 2 * core
    my_part = pl.ds(pl.multiple_of(t * part, part), part)

    wr, wk, wv, wd = (joined.at[pl.ds(i * HEAD_WIDTH, HEAD_WIDTH)] for i in range(4))
    units = dg_hbm.shape[0]
    dg, du = (dense_up.at[pl.ds(i * 128, units)] for i in range(2))
    sources = (
        tokens_hbm, gain1_hbm, wr_hbm, wk_hbm, wv_hbm, wd_hbm, doff_hbm, coff_hbm, ckey_hbm, own_hbm, hgain_hbm,
        state_hbm, wout_hbm, routes_hbm, rweight_hbm, gain2_hbm, eg_hbm, eu_hbm, dg_hbm, du_hbm, ed_hbm, dd_hbm, goff_hbm,
    )
    targets = (
        tok, gain1, wr, wk, wv, wd, doff, coff, ckey, own, hgain,
        state, wout, routes, rweight, gain2, eg, eu, dg, du, ed, dd, goff,
    )
    loads = {
        id(to): pltpu.make_async_copy(frm, to, load_sem.at[i])
        for i, (frm, to) in enumerate(zip(sources, targets))
    }
    for to in targets[:6]:
        loads[id(to)].start()

    barrier = pltpu.get_barrier_semaphore()


    def greet(peer_group, peer_lane):
        pl.semaphore_signal(barrier, inc=1, device_id=(peer_group, peer_lane), device_id_type=MESH)

    for distance in sorted(range(1, chips), key=lambda d: -min(d, chips - d)):
        greet(lax.rem(chip + distance, chips) * 2 + 1, t)
    greet(partner, t)
    for p in range(1, lanes):
        greet(2 * chip, lax.rem(t + p, lanes))

    for to in targets[6:]:
        loads[id(to)].start()

    def arrived(*buffers):
        for to in buffers:
            loads[id(to)].wait()

    side_length = round(lanes**0.5)
    offsets = sorted(
        range(1, lanes),
        key=lambda p: -sum(min(d, side_length - d) for d in divmod(p, side_length)),
    )

    def lane_at(p):
        dy, dx = divmod(p, side_length)
        y, x = t // side_length, lax.rem(t, side_length)
        return lax.rem(y + dy, side_length) * side_length + lax.rem(x + dx, side_length)

    def over_lanes(stage, source, target):
        for p in offsets:
            peer = lane_at(p)
            pltpu.make_async_remote_copy(
                src_ref=source(peer), dst_ref=target, send_sem=send_sem.at[stage],
                recv_sem=recv_sem.at[stage], device_id=(g, peer), device_id_type=MESH,
            ).start()

    apart = sorted(range(-(chips // 2), chips - chips // 2), key=lambda r: abs(r + 0.5))
    bounds = sorted({0, *(-(-chips * end // 16) for end in ENDS)})
    parts = len(bounds) - 1
    places = [range(bounds[k], bounds[k + 1]) for k in range(parts)]
    rows_of = [slice(2 * cap * bounds[k], 2 * cap * bounds[k + 1]) for k in range(parts)]

    def to_device(stage, source, target, peer):
        pltpu.make_async_remote_copy(
            src_ref=source, dst_ref=target, send_sem=send_sem.at[stage],
            recv_sem=recv_sem.at[stage], device_id=(peer, t), device_id_type=MESH,
        ).start()

    def device_at(distance, c):
        return lax.rem(chip + distance % chips, chips) * 2 + c

    def to_experts():
        for j in reversed(range(chips)):
            stage = DISPATCH + [j in place for place in places].index(True)
            if apart[j] == 0:
                to_device(stage, disp_send.at[partner], disp_in.at[2 * j + core], partner)
                continue
            for c in range(2):
                peer = device_at(-apart[j], c)
                to_device(stage, disp_send.at[peer], disp_in.at[2 * j + core], peer)

    def to_groups(k):
        for j in reversed(places[k]):
            if apart[j] == 0:
                to_device(RETURN, back_send.at[2 * j + 1 - core], back_in.at[g], partner)
                continue
            for c in range(2):
                to_device(RETURN, back_send.at[2 * j + c], back_in.at[g], device_at(apart[j], c))

    def over_chips(stage, source, target):
        for distance in sorted(range(1, chips), key=lambda d: -min(d, chips - d)):
            peer = lax.rem(chip + distance, chips)
            to_device(stage, source(peer), target, 2 * peer + core)

    def descriptor(stage, ref):
        return pltpu.make_async_remote_copy(
            src_ref=ref, dst_ref=ref, send_sem=send_sem.at[stage], recv_sem=recv_sem.at[stage],
            device_id=(g, lax.rem(t + 1, lanes)), device_id_type=MESH,
        )

    arrived(tok, gain1)
    floats = tok[...].astype(F32)
    normed = (
        floats * lax.rsqrt(jnp.mean(floats * floats, axis=-1, keepdims=True) + 1e-06) * gain1[...]
    ).astype(BF16)
    arrived(wr, wk, wv, wd)
    projected = lax.dot_general(normed, joined[...], (((1,), (1,)), ((), ())), preferred_element_type=F32)
    recept = projected[:, 0:HEAD_WIDTH]
    keys = projected[:, HEAD_WIDTH : 2 * HEAD_WIDTH]
    values = projected[:, 2 * HEAD_WIDTH : 3 * HEAD_WIDTH]
    decay_pre = projected[:, 3 * HEAD_WIDTH : 4 * HEAD_WIDTH]

    arrived(doff, coff, ckey, own, hgain)
    decay = jnp.exp(-jnp.exp(doff[...] + decay_pre))
    rate = sigmoid(coff[...] + ckey[...] * keys)
    key_in = keys * rate
    unit = keys * lax.rsqrt(jnp.mean(keys * keys, axis=-1, keepdims=True) + 1e-06) * HEAD_WIDTH**-0.5

    def twice(x):
        return jnp.concatenate([x, x], axis=1)

    decay2, unit2, rate2, key2, recept2, values2 = map(
        twice, (decay, unit, unit * rate, key_in, recept, values)
    )
    lane_of = lax.broadcasted_iota(jnp.int32, (seqs, pair), 1)
    low = lane_of < HEAD_WIDTH

    def halves(x):
        first = jnp.sum(jnp.where(low, x, 0.0), axis=-1, keepdims=True)
        second = jnp.sum(jnp.where(low, 0.0, x), axis=-1, keepdims=True)
        return first, second

    def picked(x, lane):
        return jnp.sum(jnp.where(lane_of == lane, x, 0.0), axis=-1, keepdims=True)

    arrived(state)
    at_once = 4

    def some_tiles(step, readout):
        for inner in range(at_once):
            c = step * at_once + inner
            rows = pl.ds(c, seqs, stride=tiles)
            block = state[rows, :]
            removed = jnp.where(low, *halves(block * unit2))
            added = jnp.where(low, picked(values2, 2 * c), picked(values2, 2 * c + 1))
            block = block * decay2 - removed * rate2 + added * key2
            next_state[rows, :] = block
            first, second = halves(block * recept2)
            readout = jnp.where(lane_of == 2 * c, first, readout)
            readout = jnp.where(lane_of == 2 * c + 1, second, readout)
        return readout

    readout = lax.fori_loop(0, tiles // at_once, some_tiles, jnp.zeros((seqs, pair), F32))
    readout = readout[:, 0:HEAD_WIDTH]
    center = jnp.mean(readout, axis=-1, keepdims=True)
    spread = jnp.mean(jnp.square(readout - center), axis=-1, keepdims=True)
    heads = (readout - center) * lax.rsqrt(spread + 0.00064) * hgain[...]
    heads = heads + jnp.sum(recept * key_in * own[...], axis=-1, keepdims=True) * values
    heads = heads.astype(BF16)

    arrived(wout)
    share = jnp.dot(heads, wout[...], preferred_element_type=F32)
    wide[0:seqs, :] = share
    col_send[...] = share.astype(BF16)
    col_in[pl.ds(t, 1)] = col_send[:, my_part][None]
    @pl.when(core == 0)
    def _():
        pl.semaphore_wait(barrier, 2 * lanes - 1)
        pl.semaphore_signal(go, inc=1, device_id=(partner, t), device_id_type=MESH)

    @pl.when(core == 1)
    def _():
        pl.semaphore_wait(go, 1)

    over_lanes(
        COLUMNS, lambda peer: col_send.at[:, pl.ds(pl.multiple_of(peer * part, part), part)], col_in.at[t]
    )
    for p in range(lanes):
        row_send[p] = wide[p * per_lane : (p + 1) * per_lane, :].astype(BF16)
    row_in[pl.ds(t, 1)] = row_send[pl.ds(t, 1)]
    over_lanes(ROWS, lambda peer: row_send.at[peer], row_in.at[t])
    mine = (
        lax.broadcasted_iota(jnp.int32, (per_lane, seqs), 1)
        == lax.broadcasted_iota(jnp.int32, (per_lane, seqs), 0) + t * per_lane
    ).astype(BF16)
    hidden[...] = jnp.dot(mine, tok[...], preferred_element_type=F32)

    arrived(routes, rweight)
    chunk = pl.ds(pl.multiple_of(g // (128 // seqs) * 128, 128), 128)
    offset = lax.rem(g, 128 // seqs) * seqs
    pick = (
        lax.broadcasted_iota(jnp.int32, (128, seqs), 0)
        == lax.broadcasted_iota(jnp.int32, (128, seqs), 1) + offset
    ).astype(BF16)
    own_routes = jnp.dot(
        routes[:, chunk].astype(F32).astype(BF16), pick, preferred_element_type=F32
    ).astype(jnp.int32)
    slot = lax.broadcasted_iota(jnp.int32, (experts * cap, seqs), 0)
    expert_of, place_of = slot // cap, lax.rem(slot, cap)
    first, second = own_routes[0:1] == expert_of, own_routes[1:2] == expert_of
    either = jnp.where(first | second, 1.0, 0.0).astype(BF16)
    earlier = (
        lax.broadcasted_iota(jnp.int32, (seqs, seqs), 0)
        < lax.broadcasted_iota(jnp.int32, (seqs, seqs), 1)
    ).astype(BF16)
    here = jnp.dot(either, earlier, preferred_element_type=F32).astype(jnp.int32) == place_of
    table = jnp.where((first | second) & here, 1.0, 0.0).astype(BF16)
    weighted = jnp.where(first & here, rweight[0:1], 0.0) + jnp.where(second & here, rweight[1:2], 0.0)

    arrived(gain2)
    descriptor(COLUMNS, col_in.at[pl.ds(0, lanes - 1)]).wait_recv()
    total = tok[:, my_part].astype(F32)
    for p in range(lanes):
        total = total + col_in[p].astype(F32)
    gained = (total * gain2[:, my_part]).astype(BF16)
    slots[...] = jnp.dot(table, gained, preferred_element_type=F32)
    for e in range(experts):
        disp_send[e] = slots[e * cap : (e + 1) * cap, :].astype(BF16)
    disp_in[pl.ds(2 * apart.index(0) + core, 1)] = disp_send[pl.ds(g, 1)]

    @pl.when(core == 1)
    def _():
        pl.semaphore_wait(barrier, 2 * chips - 1)
        pl.semaphore_signal(go, inc=1, device_id=(partner, t), device_id_type=MESH)

    @pl.when(core == 0)
    def _():
        pl.semaphore_wait(go, 1)

    to_experts()

    descriptor(ROWS, row_in.at[pl.ds(0, lanes - 1)]).wait_recv()
    total = hidden[...]
    for p in range(lanes):
        total = total + row_in[p].astype(F32)
    hidden[...] = total
    dense_send[...] = (
        total * lax.rsqrt(jnp.mean(total * total, axis=-1, keepdims=True) + 1e-06) * gain2[...]
    ).astype(BF16)
    dense_in[pl.ds(core * chips + chip, 1)] = dense_send[...][None]
    over_chips(DENSE, lambda peer: dense_send, dense_in.at[core * chips + chip])

    def whole_rows(k):
        rows = rows_of[k]
        for e in range(rows.start // cap, rows.stop // cap):
            slots[e * cap : (e + 1) * cap, :] = disp_in[e].astype(F32)
        rows_all[rows, my_part] = slots[rows, :].astype(BF16)
        mine = rows_all.at[rows, my_part]
        over_lanes(GATHER + k, lambda peer: mine, mine)

    packets = [2 * len(places[k]) - (k == 0) for k in range(parts)]
    for k in range(parts):
        descriptor(DISPATCH + k, disp_in.at[pl.ds(0, packets[k])]).wait_recv()
        whole_rows(k)

    inverse = 1.0 / (gain2[...] * gain2[...])

    def expert(k):
        rows = rows_of[k]
        squares = jnp.zeros((rows.stop - rows.start, part), F32)
        for p in range(lanes):
            piece = rows_all[rows, p * part : (p + 1) * part].astype(F32)
            squares = squares + piece * piece * inverse[:, p * part : (p + 1) * part]
        scale = lax.rsqrt(jnp.sum(squares, axis=-1, keepdims=True) / width + 1e-06)
        gate = jnp.dot(rows_all[rows, :], eg[0], preferred_element_type=F32) * scale
        up = jnp.dot(rows_all[rows, :], eu[0], preferred_element_type=F32) * scale
        inner = (gate * sigmoid(gate) * up).astype(BF16)
        block = 2 * part
        for p in range(width // block):
            eo_send[rows, p * block : (p + 1) * block] = jnp.dot(
                inner, ed[0, :, p * block : (p + 1) * block], preferred_element_type=F32
            ).astype(BF16)
        eo_in[pl.ds(t, 1), rows] = eo_send[rows, my_part][None]
        over_lanes(
            SUMS + k,
            lambda peer: eo_send.at[rows, pl.ds(pl.multiple_of(peer * part, part), part)],
            eo_in.at[t, rows],
        )

    my_half, other_half = pl.ds(core * chips, chips), pl.ds((1 - core) * chips, chips)
    descriptor(DENSE, dense_in.at[pl.ds(0, chips - 1)]).wait_recv()
    to_device(PASS_ON, dense_in.at[my_half], dense_in.at[my_half], partner)

    gathered = [rows_all.at[rows, pl.ds(0, width - part)] for rows in rows_of]
    arrived(eg, eu, ed)
    descriptor(GATHER, gathered[0]).wait_recv()
    expert(0)

    arrived(dg, du, dd, goff)
    descriptor(PASS_ON, dense_in.at[pl.ds(0, chips)]).wait_recv()
    for e in range(groups):
        wide[e * per_lane : (e + 1) * per_lane, :] = dense_in[e].astype(F32)
    dense_rows[...] = wide[...].astype(BF16)
    both = lax.dot_general(
        dense_rows[...], dense_up[...], (((1,), (1,)), ((), ())), preferred_element_type=F32
    )
    gate, up = both[:, 0:units], both[:, 128 : 128 + units]
    inner = (gate * sigmoid(gate) * up).astype(BF16)
    wide[...] = jnp.dot(inner, dd[...], preferred_element_type=F32)
    for e in range(groups):
        dback_send[e] = wide[e * per_lane : (e + 1) * per_lane, :].astype(BF16)
    to_device(PAIR, dback_send.at[other_half], pair_in, partner)

    def dense_sums_out():
        descriptor(PAIR, pair_in).wait_recv()
        chip_sum[...] = (dback_send[my_half].astype(F32) + pair_in[...].astype(F32)).astype(BF16)
        dback_in[pl.ds(chip, 1)] = chip_sum[pl.ds(chip, 1)]
        over_chips(BLOCKS, lambda peer: chip_sum.at[peer], dback_in.at[chip])

    for k in range(1, parts):
        descriptor(GATHER + k, gathered[k]).wait_recv()
        expert(k)
        if k == 1:
            dense_sums_out()

    def expert_sums(k):
        rows = rows_of[k]
        total = jnp.zeros((rows.stop - rows.start, part), F32)
        for p in range(lanes):
            total = total + eo_in[p, rows].astype(F32)
        slots[rows, :] = total
        for e in range(rows.start // cap, rows.stop // cap):
            back_send[e] = slots[e * cap : (e + 1) * cap, :].astype(BF16)

    summed = [eo_in.at[pl.ds(0, lanes - 1), rows] for rows in rows_of]
    for k in range(parts):
        descriptor(SUMS + k, summed[k]).wait_recv()
        expert_sums(k)
        if k == 0:
            back_in[pl.ds(g, 1)] = back_send[pl.ds(2 * apart.index(0) + core, 1)]
        to_groups(k)

    upper = weighted.astype(BF16)
    lower = (weighted - upper.astype(F32)).astype(BF16)
    descriptor(RETURN, back_in.at[pl.ds(0, groups - 1)]).wait_recv()
    for e in range(experts):
        slots[e * cap : (e + 1) * cap, :] = back_in[e].astype(F32)
    back = slots[...].astype(BF16)
    across = (((0,), (0,)), ((), ()))
    moe = lax.dot_general(upper, back, across, preferred_element_type=F32)
    moe = moe + lax.dot_general(lower, back, across, preferred_element_type=F32)
    slots[0:seqs, :] = moe
    for p in range(lanes):
        moe_send[p] = slots[p * per_lane : (p + 1) * per_lane, :]
    moe_in[pl.ds(t, 1)] = moe_send[pl.ds(t, 1)]
    over_lanes(FINAL, lambda peer: moe_send.at[peer], moe_in.at[t])

    descriptor(BLOCKS, dback_in.at[pl.ds(0, chips - 1)]).wait_recv()
    total = jnp.zeros((per_lane, width), F32)
    for e in range(chips):
        total = total + dback_in[e].astype(F32)
    total = hidden[...] + sigmoid(goff[...]) * total
    descriptor(FINAL, moe_in.at[pl.ds(0, lanes - 1)]).wait_recv()
    for p in range(lanes):
        moe_wide[:, p * part : (p + 1) * part] = moe_in[p]
    out_ref[...] = (total + moe_wide[...]).astype(BF16)

    sent = {
        COLUMNS: col_in.at[pl.ds(0, lanes - 1)],
        ROWS: row_in.at[pl.ds(0, lanes - 1)],
        DENSE: dense_in.at[pl.ds(0, chips - 1)],
        PASS_ON: dense_in.at[pl.ds(0, chips)],
        PAIR: pair_in,
        BLOCKS: dback_in.at[pl.ds(0, chips - 1)],
        RETURN: back_in.at[pl.ds(0, groups - 1)],
        FINAL: moe_in.at[pl.ds(0, lanes - 1)],
    }
    for k in range(parts):
        sent |= {DISPATCH + k: disp_in.at[pl.ds(0, packets[k])], GATHER + k: gathered[k], SUMS + k: summed[k]}
    for stage, ref in sent.items():
        descriptor(stage, ref).wait_send()


def finish_kernel(out_vmem, next_vmem, out_hbm, next_hbm, sems):
    copies = (
        pltpu.make_async_copy(next_vmem, next_hbm, sems.at[0]),
        pltpu.make_async_copy(out_vmem, out_hbm, sems.at[1]),
    )
    for copy in copies:
        copy.start()
    for copy in copies:
        copy.wait()


def local(*args):
    (
        tokens, state, gain1, wr, wk, wv, wd, doff, coff, ckey, own, hgain, wout, gain2,
        routing, rweight, eg, eu, ed, dg, du, dd, goff,
    ) = args
    groups, lanes = lax.axis_size("ep"), lax.axis_size("tp")
    seqs, width = tokens.shape
    top = routing.shape[1]
    experts = groups
    cap = 2 * seqs * top // experts
    per_lane, part = seqs // lanes, width // lanes
    rows = seqs * HEAD_WIDTH * HEAD_WIDTH // 128
    row = lambda v: v.reshape(1, -1)
    operands = (
        tokens, state.reshape(rows, 128), row(gain1), wr.T, wk.T, wv.T, wd.T, row(doff), row(coff), row(ckey), row(own),
        row(hgain), wout, row(gain2), routing.T, rweight.T, eg, eu, ed, dg.T, du.T, dd, row(goff),
    )
    vmem = pltpu.VMEM
    joined, dense_up = vmem((4 * HEAD_WIDTH, width), BF16), vmem((256, width), BF16)
    held = [vmem(a.shape, a.dtype) for a in operands]
    held = [*held[:3], joined, *held[7:19], dense_up, *held[21:]]
    sizes = (groups, lanes, seqs, width, experts, cap)
    scratch = held + [
        vmem((groups * per_lane, width), F32),
        vmem((groups * cap, part), F32),
        vmem((seqs, width), BF16),
        vmem((lanes, per_lane, width), BF16),
        vmem((lanes, seqs, part), BF16),
        vmem((lanes, per_lane, width), BF16),
        vmem((per_lane, width), F32),
        vmem((experts, cap, part), BF16),
        vmem((groups, cap, part), BF16),
        vmem((groups * cap, width), BF16),
        vmem((per_lane, width), BF16),
        vmem((groups, per_lane, width), BF16),
        vmem((groups * per_lane, width), BF16),
        vmem((groups, per_lane, width), BF16),
        vmem((groups // 2, per_lane, width), BF16),
        vmem((groups // 2, per_lane, width), BF16),
        vmem((groups // 2, per_lane, width), BF16),
        vmem((groups * cap, width), BF16),
        vmem((lanes, groups * cap, part), BF16),
        vmem((groups, cap, part), BF16),
        vmem((experts, cap, part), BF16),
        vmem((lanes, per_lane, part), F32),
        vmem((lanes, per_lane, part), F32),
        vmem((per_lane, width), F32),
        pltpu.SemaphoreType.DMA((len(operands),)),
        pltpu.SemaphoreType.DMA((STAGES,)),
        pltpu.SemaphoreType.DMA((STAGES,)),
        pltpu.SemaphoreType.REGULAR,
    ]
    layer_out, next_state = pl.pallas_call(
        functools.partial(layer_kernel, sizes),
        out_shape=(vmem((per_lane, width), BF16), vmem((rows, 128), F32)),
        in_specs=[pl.BlockSpec(memory_space=pltpu.HBM)] * len(operands),
        out_specs=[pl.BlockSpec(memory_space=pltpu.VMEM)] * 2,
        scratch_shapes=scratch,
        compiler_params=pltpu.CompilerParams(
            collective_id=0, has_side_effects=True, vmem_limit_bytes=60_000_000
        ),
        name="layer",
    )(*operands)
    layer_out, next_state = pl.pallas_call(
        finish_kernel,
        out_shape=(
            jax.ShapeDtypeStruct((per_lane, width), BF16),
            jax.ShapeDtypeStruct((rows, 128), F32),
        ),
        in_specs=[pl.BlockSpec(memory_space=pltpu.VMEM)] * 2,
        out_specs=[pl.BlockSpec(memory_space=pltpu.HBM)] * 2,
        scratch_shapes=[pltpu.SemaphoreType.DMA((2,))],
        compiler_params=pltpu.CompilerParams(vmem_limit_bytes=2_000_000),
        name="finish",
    )(layer_out, next_state)
    return layer_out, next_state.reshape(state.shape)


def solution(mesh):
    return jax.shard_map(
        local,
        mesh=mesh,
        in_specs=(
            P("ep", None),
            P("ep", "tp", None),
            P(),
            P(None, "tp"),
            P(None, "tp"),
            P(None, "tp"),
            P(None, "tp"),
            P("tp"),
            P("tp"),
            P("tp"),
            P("tp"),
            P("tp"),
            P("tp", None),
            P(),
            P(),
            P("ep", None),
            P("ep", None, "tp"),
            P("ep", None, "tp"),
            P("ep", "tp", None),
            P(None, "ep"),
            P(None, "ep"),
            P("ep", None),
            P(),
        ),
        out_specs=(P(("ep", "tp"), None), P("ep", "tp", None)),
        check_vma=False,
    )
```
